32 devices in a mesh: grp: 2 (over y), dp: 2 (over x), kv: 4 (over z), tp: 2 (over core).
Axes of the slice: x: 2, y: 2, z: 4, core: 2. Of those that a mesh axis runs over, the one named last changes fastest.
Arguments:
- tokens: bfloat16 [32, 2048], P(('grp', 'dp'), 'kv'), parts along dimension 0, may hold values from -110 to 110
- attend_gain: float32 [2048], P('kv'), may hold values from 0.1 to 1.9
- query_weight: bfloat16 [2048, 2048], P('kv', 'tp'), may hold values from -0.125 to 0.125
- cache_keys: bfloat16 [32, 1536, 2, 128], P(('grp', 'dp'), 'kv', 'tp'), parts along dimension 0, may hold values from -1600 to 1600
- cache_values: bfloat16 [32, 1536, 2, 128], P(('grp', 'dp'), 'kv', 'tp'), parts along dimension 0, may hold values from -6 to 6
- head_lambda: float32 [16], P('tp'), may hold values from 0.3 to 0.8
- head_gain: float32 [128], replicated, may hold values from 0.1 to 1.9
- output_weight: bfloat16 [2048, 2048], P('tp', 'kv'), may hold values from -0.125 to 0.125
- mixer_gain: float32 [2048], P('kv'), may hold values from 0.1 to 1.9
- gate_weight: bfloat16 [2048, 5632], P('kv', 'tp'), may hold values from -0.125 to 0.125
- up_weight: bfloat16 [2048, 5632], P('kv', 'tp'), may hold values from -0.125 to 0.125
- down_weight: bfloat16 [5632, 2048], P('tp', 'kv'), may hold values from -0.078125 to 0.078125
Outputs:
- layer_out: bfloat16 [32, 2048], P(('grp', 'dp'), 'kv'), parts along dimension 0
The draws below stay inside these ranges and needn't reach their ends.
There are 2 independent parts, one for each index of `grp`. The reference program is written for one: setup_inputs(seed, part) draws one part's arguments, and reference() takes and returns one part's arrays. A program takes and returns all parts, laid end to end along the dimension named above; an argument that names none is the same for every part. Nothing has to cross between parts.
All inputs are finite; a program needn't handle non-finite values.
Results may differ from the reference program's by a relative error of at most 0.025.
Values may be sent and summed in bfloat16 or wider, within the bound.
A program may use at most 64 MiB of HBM per device.

```python
import jax
import jax.numpy as jnp
from jax import lax

D = 2048
H = 16
KVH = 2
HD = 64
VD = 128
FF = 5632
GROUP = 8
BATCH = 16
CTX = 1536
N_TP = 2


def draw_tokens(key, part):
    columns = jnp.arange(D, dtype=jnp.float32)
    column_scale = 0.4 * 10.0 ** (columns / D)
    roughness = jax.random.uniform(jax.random.fold_in(key, 1), (D,), jnp.float32, 0.5, 1.5)
    values = jnp.clip(jax.random.normal(key, (BATCH, D), jnp.float32), -6.0, 6.0)
    return (values * column_scale * roughness).astype(jnp.bfloat16)


def draw_cache_keys(key, part):
    drawn = jnp.clip(jax.random.normal(key, (BATCH, CTX, KVH, 2 * HD), jnp.float32), -6.0, 6.0) * 1.7
    return drawn.astype(jnp.bfloat16)


def levels(key, dims, split, smallest, high):
    level = 1.0
    for dim, parts in split:
        draws = jax.random.uniform(jax.random.fold_in(jax.random.fold_in(key, 6), dim), (parts,), jnp.float32, smallest / len(split), high / len(split))
        level = level * jnp.repeat(jnp.exp(draws), dims[dim] // parts).reshape((-1,) + (1,) * (len(dims) - 1 - dim))
    return level


def noise(stream_key, shape, deviation, most, cuts=(), kind=jnp.bfloat16):
    values = jax.random.normal(stream_key, shape, jnp.float32) * deviation
    if len(cuts) > 0:
        values = levels(stream_key, shape, cuts, -0.22, 0.18) * values
    return jnp.clip(values, min=-most, max=most).astype(kind)


def setup_inputs(seed: int = 0, part: int = 0) -> dict:
    key_list = jax.random.split(jax.random.key(seed), 13)
    own_keys = jax.random.split(jax.random.fold_in(key_list[12], part), 13)
    return {
        "tokens": draw_tokens(jax.random.fold_in(jax.random.fold_in(key_list[12], part), 71), part),
        "attend_gain": jnp.clip(1.0 + 0.18 * jax.random.normal(key_list[1], (D,), jnp.float32), 0.1, 1.9),
        "query_weight": noise(key_list[2], (D, H * 2 * HD), D ** -0.5, 0.125, ((0, 4), (1, 2))),
        "cache_keys": draw_cache_keys(jax.random.fold_in(jax.random.fold_in(key_list[12], part), 71), part),
        "cache_values": noise(own_keys[4], (BATCH, CTX, KVH, VD), 1.0, 6.0, ((0, 2), (1, 4), (2, 2))),
        "head_lambda": jnp.clip(0.3 + 0.5 * jax.random.uniform(key_list[5], (H,), jnp.float32) ** levels(key_list[5], (H,), ((0, 2),), -0.2, 0.2), 0.3, 0.8),
        "head_gain": jnp.clip(1.0 + 0.18 * jax.random.normal(key_list[6], (VD,), jnp.float32), 0.1, 1.9),
        "output_weight": noise(key_list[7], (H * VD, D), (H * VD) ** -0.5, 0.125, ((0, 2), (1, 4))),
        "mixer_gain": jnp.clip(1.0 + 0.18 * jax.random.normal(key_list[8], (D,), jnp.float32), 0.1, 1.9),
        "gate_weight": noise(key_list[9], (D, FF), D ** -0.5, 0.125, ((0, 4), (1, 2))),
        "up_weight": noise(key_list[10], (D, FF), D ** -0.5, 0.125, ((0, 4), (1, 2))),
        "down_weight": noise(key_list[11], (FF, D), FF ** -0.5, 0.078125, ((0, 2), (1, 4))),
    }


ROPE_BASE = 500000.0
EPSILON = 1e-06
KEEP_SCALE = 0.8

def rotate(query, position):
    half_dim = query.shape[-1] // 2
    frequency = ROPE_BASE ** (-jnp.arange(half_dim, dtype=jnp.float32) * 2.0 / query.shape[-1])
    angles = position * frequency
    cosine_part = jnp.cos(angles)
    sine_part = jnp.sin(angles)
    first_half = query[..., :half_dim]
    second_half = query[..., half_dim:]
    return jnp.concatenate([first_half * cosine_part - second_half * sine_part, second_half * cosine_part + first_half * sine_part], axis=-1)

def group_sum(left, right, pieces):
    width = left.shape[1] // pieces
    running = jnp.zeros((left.shape[0], right.shape[1]), jnp.float32)
    for block_index in range(pieces):
        product = jnp.dot(left[:, block_index * width:(block_index + 1) * width], right[block_index * width:(block_index + 1) * width], preferred_element_type=jnp.float32)
        rounded = lax.optimization_barrier(product.astype(jnp.bfloat16))
        running = running + rounded.astype(jnp.float32)
    return running

def attend(arrays):
    query_row, key_row, value_row = arrays
    scores = jnp.einsum('kgcd,pkcd->kgcp', query_row.astype(jnp.float32), key_row.astype(jnp.float32)) * HD ** (-0.5)
    row_max = lax.optimization_barrier(jnp.max(scores, axis=-1, keepdims=True))
    exponent = jnp.exp(scores - row_max)
    row_total = lax.optimization_barrier(jnp.sum(exponent, axis=-1))
    rounded = lax.optimization_barrier(exponent.astype(jnp.bfloat16))
    weighted = jnp.einsum('kgcp,pke->kgce', rounded.astype(jnp.float32), value_row.astype(jnp.float32))
    return weighted / row_total[..., None]

def reference(tokens, attend_gain, query_weight, cache_keys, cache_values, head_lambda, head_gain, output_weight, mixer_gain, gate_weight, up_weight, down_weight):
    tok_float = tokens.astype(jnp.float32)
    scaled = (tok_float * attend_gain).astype(jnp.bfloat16)
    attend_scale = lax.rsqrt(lax.optimization_barrier(jnp.mean(tok_float * tok_float, axis=1, keepdims=True)) + EPSILON)
    query = attend_scale * jnp.dot(scaled, query_weight, preferred_element_type=jnp.float32)
    query = rotate(query.reshape(BATCH, KVH, GROUP, 2, HD), jnp.asarray(CTX, jnp.float32))
    query = lax.optimization_barrier(query.astype(jnp.bfloat16))
    key_block = cache_keys.reshape(BATCH, CTX, KVH, 2, HD)
    averaged = lax.map(attend, (query, key_block, cache_values))
    lambda_grid = head_lambda.reshape(KVH, GROUP)[None, :, :, None]
    difference = averaged[:, :, :, 0] - lambda_grid * averaged[:, :, :, 1]
    normed = difference * lax.rsqrt(lax.optimization_barrier(jnp.mean(difference * difference, axis=-1, keepdims=True)) + EPSILON)
    heads_out = (normed * head_gain * KEEP_SCALE).astype(jnp.bfloat16).reshape(BATCH, H * VD)
    middle = (tok_float + group_sum(heads_out, output_weight, N_TP)).astype(jnp.bfloat16)
    mid_float = middle.astype(jnp.float32)
    mixer_in = (mid_float * mixer_gain).astype(jnp.bfloat16)
    mixer_scale = lax.rsqrt(lax.optimization_barrier(jnp.mean(mid_float * mid_float, axis=1, keepdims=True)) + EPSILON)
    gate = mixer_scale * jnp.dot(mixer_in, gate_weight, preferred_element_type=jnp.float32)
    up_value = mixer_scale * jnp.dot(mixer_in, up_weight, preferred_element_type=jnp.float32)
    hidden = (jax.nn.silu(gate) * up_value).astype(jnp.bfloat16)
    mixed = group_sum(hidden, down_weight, N_TP)
    return (mid_float + mixed).astype(jnp.bfloat16)
```

```python
import functools

import jax
import jax.numpy as jnp
import numpy as np
from jax import lax
from jax.experimental import pallas as pl
from jax.experimental.pallas import tpu as pltpu
from jax.sharding import PartitionSpec as P

HD = 64
ROPE_BASE = 500000.0
EPSILON = 1e-06
KEEP_SCALE = 0.8
LANES = 128
B_PARTS = 2
F32 = jnp.float32
BF16 = jnp.bfloat16


def high_low(column):
    high = column.astype(BF16).astype(F32)
    low = column - high
    lane = lax.broadcasted_iota(jnp.int32, (column.shape[0], LANES), 1)
    return jnp.where(lane < LANES // 2, high, low).astype(BF16)


def from_high_low(tile):
    tile = tile.astype(F32)
    return tile[:, 0:1] + tile[:, LANES // 2 : LANES // 2 + 1]


def kernel(
    n_kv,
    n_tp,
    n_pieces,
    widths,
    features,
    tok_hbm,
    again_hbm,
    wq_hbm,
    key_hbm,
    val_hbm,
    lam_hbm,
    hgain_hbm,
    wo_hbm,
    mgain_hbm,
    wg_hbm,
    wu_hbm,
    wd_hbm,
    rope_hbm,
    out_ref,
    tok,
    again,
    wq,
    keys,
    vals,
    lam,
    hgain,
    wo,
    mgain,
    wg,
    wu,
    wd,
    rope,
    a_send,
    a_recv,
    b_send,
    b_recv,
    s_send,
    s_recv,
    c_send,
    c_recv,
    d_sends,
    d_recvs,
    e_alls,
    f_send,
    f_recv,
    query_rows,
    head_rows,
    load_sem,
    kv_send,
    kv_recv,
    piece_send,
    tp_send,
    tp_recv,
):
    me = lax.axis_index("kv")
    core = lax.axis_index("tp")
    rows = tok.shape[0]
    heads = lam.shape[1]
    hidden_here = wg_hbm.shape[1]

    loads = []
    for index, (source, target) in enumerate(
        [
            (tok_hbm, tok),
            (again_hbm, again),
            (wq_hbm, wq),
            (rope_hbm, rope),
            (lam_hbm, lam),
            (hgain_hbm, hgain),
            (mgain_hbm, mgain),
            (key_hbm, keys),
            (val_hbm, vals),
            (wo_hbm, wo),
            (wg_hbm, wg),
            (wu_hbm, wu),
            (wd_hbm, wd),
        ]
    ):
        copy = pltpu.make_async_copy(source, target, load_sem.at[index])
        copy.start()
        loads.append(copy)

    barrier = pltpu.get_barrier_semaphore()
    for k in range(1, n_kv):
        pl.semaphore_signal(
            barrier,
            inc=1,
            device_id={"kv": lax.rem(me + k, n_kv)},
            device_id_type=pl.DeviceIdType.MESH,
        )
    for k in range(1, n_tp):
        pl.semaphore_signal(
            barrier,
            inc=1,
            device_id={"tp": lax.rem(core + k, n_tp)},
            device_id_type=pl.DeviceIdType.MESH,
        )

    pending = []
    half = max(n_kv // 2, 1)
    on_left = me < half

    def far_first(j):
        below, above = n_kv - 1 - j, j
        below = jnp.where(below > me, below, below - 1)
        above = jnp.where(above < me, above, above + 1)
        return jnp.where(on_left, below, above)

    peers = [far_first(j) for j in range(n_kv - 1)]

    def kv_copy(phase, source, target, slot_sent, slot_received, peer):
        return pltpu.make_async_remote_copy(
            src_ref=source,
            dst_ref=target,
            send_sem=kv_send.at[phase, slot_sent],
            recv_sem=kv_recv.at[phase, slot_received],
            device_id={"kv": peer},
            device_id_type=pl.DeviceIdType.MESH,
        )

    def to_all(phase, source, landing):
        for j, peer in enumerate(peers):
            copy = kv_copy(phase, source, landing(me), j, me, peer)
            copy.start()
            pending.append(copy)

    def from_kv(phase, landing, origin):
        kv_copy(phase, landing, landing, 0, origin, origin).wait_recv()

    def to_tp(phase, k, source, target):
        copy = pltpu.make_async_remote_copy(
            src_ref=source,
            dst_ref=target,
            send_sem=tp_send.at[phase, k - 1],
            recv_sem=tp_recv.at[phase, k - 1],
            device_id={"tp": lax.rem(core + k, n_tp)},
            device_id_type=pl.DeviceIdType.MESH,
        )
        copy.start()
        pending.append(copy)
        return copy

    for index in (0, 1, 2):
        loads[index].wait()
    tok_float = tok[...].astype(F32)
    scaled = (tok_float * again[...]).astype(BF16)
    query_part = jnp.dot(scaled, wq[...], preferred_element_type=F32)
    squares = jnp.sum(tok_float * tok_float, axis=1, keepdims=True)
    query_width = wq.shape[1]
    a_send[:, :query_width] = query_part.astype(BF16)
    a_send[:, query_width:] = high_low(squares)
    pl.semaphore_wait(barrier, n_kv - 1 + n_tp - 1)
    to_all(0, a_send, lambda slot: a_recv.at[slot])
    for index in (3, 4, 5, 6, 7):
        loads[index].wait()
    for peer in reversed(peers):
        from_kv(0, a_recv.at[peer], peer)
        query_part = query_part + a_recv[peer, :, :query_width].astype(F32)
        squares = squares + from_high_low(a_recv[peer, :, query_width:])
    query = query_part * lax.rsqrt(squares / features + EPSILON)

    lane = lax.broadcasted_iota(jnp.int32, (rows, LANES), 1)
    lower = lax.rem(lane, HD) < HD // 2
    cosine = rope[0:1, :]
    sine = rope[1:2, :]
    for h in range(heads):
        block = query[:, h * LANES : (h + 1) * LANES]
        partner = jnp.where(
            lower,
            pltpu.roll(block, LANES - HD // 2, 1),
            pltpu.roll(block, HD // 2, 1),
        )
        query_rows[h * rows : (h + 1) * rows, :] = block * cosine + partner * sine

    head_lane = lax.broadcasted_iota(jnp.int32, (heads, LANES), 1)
    scores = []
    for b in range(rows):
        turned = query_rows[pl.ds(b, heads, stride=rows), :]
        rounded = turned.astype(BF16).astype(F32) * HD ** (-0.5)
        both = jnp.concatenate(
            [
                jnp.where(head_lane < HD, rounded, 0.0),
                jnp.where(head_lane < HD, 0.0, rounded),
            ],
            axis=0,
        ).astype(BF16)
        scores.append(
            lax.dot_general(
                both, keys[b], (((1,), (1,)), ((), ())), preferred_element_type=F32
            )
        )
    loads[8].wait()
    count = 2 * heads
    all_rows = rows * count
    weighted, row_max, row_total = [], [], []
    for b in range(rows):
        top = jnp.max(scores[b], axis=1, keepdims=True)
        exponent = jnp.exp(scores[b] - top)
        row_max.append(top)
        row_total.append(jnp.sum(exponent, axis=1, keepdims=True))
        own = jnp.dot(exponent.astype(BF16), vals[b], preferred_element_type=F32)
        b_send[b * count : (b + 1) * count, :] = own.astype(BF16)
        weighted.append(own)
        if (b + 1) % (rows // B_PARTS) == 0:
            part = b // (rows // B_PARTS)
            span = pl.ds(part * (all_rows // B_PARTS), all_rows // B_PARTS)
            to_all(1 + part, b_send.at[span], lambda slot: b_recv.at[slot, span])
    diagonal = lax.broadcasted_iota(jnp.int32, (all_rows, all_rows), 0) == (
        lax.broadcasted_iota(jnp.int32, (all_rows, all_rows), 1)
    )

    def to_lanes(column):
        return jnp.sum(jnp.where(diagonal, column, 0.0), axis=0, keepdims=True)

    def to_rows(line):
        return jnp.sum(jnp.where(diagonal, line, 0.0), axis=1, keepdims=True)

    own_max = to_lanes(jnp.concatenate(row_max, axis=0))
    own_total = to_lanes(jnp.concatenate(row_total, axis=0))
    s_send[0:1, :] = own_max
    s_send[1:2, :] = own_total
    to_all(5, s_send, lambda slot: s_recv.at[slot])
    weighted = jnp.concatenate(weighted, axis=0)
    eye = lax.broadcasted_iota(jnp.int32, (heads, heads), 0) == (
        lax.broadcasted_iota(jnp.int32, (heads, heads), 1)
    )
    lam_column = jnp.sum(jnp.where(eye, lam[...], 0.0), axis=1, keepdims=True)
    for peer in reversed(peers):
        from_kv(5, s_recv.at[peer], peer)
    maxima = [own_max] + [s_recv[peer, 0:1, :] for peer in reversed(peers)]
    totals = [own_total] + [s_recv[peer, 1:2, :] for peer in reversed(peers)]
    joint = functools.reduce(jnp.maximum, maxima)
    factors = [jnp.exp(m - joint) for m in maxima]
    total = functools.reduce(jnp.add, [f * t for f, t in zip(factors, totals)])
    averaged = weighted * to_rows(factors[0] / total)
    shares = [to_rows(f / total) for f in factors[1:]]
    for share, peer in zip(shares, reversed(peers)):
        for part in range(B_PARTS):
            span = pl.ds(part * (all_rows // B_PARTS), all_rows // B_PARTS)
            from_kv(1 + part, b_recv.at[peer, span], peer)
        averaged = averaged + b_recv[peer].astype(F32) * share
    averaged = averaged.reshape(rows, 2, heads, LANES)
    difference = averaged[:, 0] - lam_column[None] * averaged[:, 1]
    normed = difference * lax.rsqrt(
        jnp.mean(difference * difference, axis=-1, keepdims=True) + EPSILON
    )
    normed = normed * (hgain[...] * KEEP_SCALE)[None]
    head_rows[...] = normed.reshape(rows * heads, LANES)
    heads_out = jnp.concatenate(
        [head_rows[pl.ds(h, rows, stride=heads), :] for h in range(heads)], axis=1
    ).astype(BF16)

    loads[9].wait()
    attended = jnp.dot(heads_out, wo[...], preferred_element_type=F32).astype(BF16)
    c_send[...] = attended
    copies = [to_tp(0, k, c_send, c_recv.at[k - 1]) for k in range(1, n_tp)]
    attended = attended.astype(F32)
    for index in (10, 11):
        loads[index].wait()
    for k, copy in enumerate(copies):
        copy.wait_recv()
        attended = attended + c_recv[k].astype(F32)
    mid_float = (tok_float + attended).astype(BF16).astype(F32)
    mixer_in = (mid_float * mgain[...]).astype(BF16)
    squares = jnp.sum(mid_float * mid_float, axis=1, keepdims=True)

    square_tile = high_low(squares)
    near = jnp.where(on_left, 0, n_pieces - 1)
    far = n_pieces - 1 - near
    first = (n_kv - n_pieces) // 2
    reduces = jnp.logical_and(me >= first, me < first + n_pieces)
    span = hidden_here // n_pieces
    starts = [sum(widths[:j]) for j in range(len(widths))]
    grids = list(zip(d_sends, d_recvs, e_alls, widths, starts))
    d_copies = []
    for piece in ([far] if n_pieces > 1 else []) + [near]:
        target = first + piece
        for j, (d_send, d_recv, _, width, start) in enumerate(grids):
            columns = pl.ds(pl.multiple_of(piece * span + start, LANES), width)
            gate = jnp.dot(mixer_in, wg[:, columns], preferred_element_type=F32)
            d_send[piece, :, :width] = gate.astype(BF16)
            up = jnp.dot(mixer_in, wu[:, columns], preferred_element_type=F32)
            d_send[piece, :, width : 2 * width] = up.astype(BF16)
            if j == 0:
                d_send[piece, :, 2 * width :] = square_tile
            copy = pltpu.make_async_remote_copy(
                src_ref=d_send.at[piece],
                dst_ref=d_recv.at[me],
                send_sem=piece_send.at[piece, j],
                recv_sem=kv_recv.at[6 + j, me],
                device_id={"kv": target},
                device_id_type=pl.DeviceIdType.MESH,
            )
            d_copies.append((target, copy))
            pl.when(me != target)(copy.start)

    e_phase = 6 + len(widths)

    @pl.when(reduces)
    def _():
        own = me - first
        row_squares = squares
        for j, (d_send, d_recv, e_all, width, _) in enumerate(grids):
            gate = d_send[own, :, :width].astype(F32)
            up = d_send[own, :, width : 2 * width].astype(F32)
            for peer in reversed(peers):
                from_kv(6 + j, d_recv.at[peer], peer)
                gate = gate + d_recv[peer, :, :width].astype(F32)
                up = up + d_recv[peer, :, width : 2 * width].astype(F32)
                if j == 0:
                    row_squares = row_squares + from_high_low(
                        d_recv[peer, :, 2 * width :]
                    )
            mixer_scale = lax.rsqrt(row_squares / features + EPSILON)
            gate = gate * mixer_scale
            up = up * mixer_scale
            e_all[own] = (gate / (1.0 + jnp.exp(-gate)) * up).astype(BF16)
            for i, peer in enumerate(peers):
                kv_copy(e_phase + j, e_all.at[own], e_all.at[own], i, own, peer).start()

    loads[12].wait()
    projected = jnp.zeros((rows, wd.shape[1]), F32)
    for j, (_, _, e_all, width, start) in enumerate(grids):
        for piece in [near] + ([far] if n_pieces > 1 else []):
            arrival = kv_copy(e_phase + j, e_all.at[piece], e_all.at[piece], 0, piece, me)
            pl.when(me != first + piece)(arrival.wait_recv)
            part = wd[pl.ds(pl.multiple_of(piece * span + start, LANES), width), :]
            projected = projected + jnp.dot(
                e_all[piece], part, preferred_element_type=F32
            )
    projected = projected.astype(BF16)
    f_send[...] = projected
    copies = [to_tp(1, k, f_send, f_recv.at[k - 1]) for k in range(1, n_tp)]
    mixed = projected.astype(F32)
    for k, copy in enumerate(copies):
        copy.wait_recv()
        mixed = mixed + f_recv[k].astype(F32)
    out_ref[...] = (mid_float + mixed).astype(BF16)
    for copy in pending:
        copy.wait_send()
    for target, copy in d_copies:
        pl.when(me != target)(copy.wait_send)

    @pl.when(reduces)
    def _():
        own = me - first
        for j, (_, _, e_all, _, _) in enumerate(grids):
            for i, peer in enumerate(peers):
                kv_copy(e_phase + j, e_all.at[own], e_all.at[own], i, own, peer).wait_send()


def rope_table(context):
    half = HD // 2
    frequency = (ROPE_BASE ** (-np.arange(half) * 2.0 / HD)).astype(np.float32)
    angles = (np.float32(context) * frequency).astype(np.float64)
    cosine = np.tile(np.cos(angles), LANES // half)
    sine = np.tile(np.concatenate([-np.sin(angles), np.sin(angles)]), LANES // HD)
    return np.stack([cosine, sine]).astype(np.float32)


def on_device(n_kv, n_tp, *arrays):
    (
        tokens,
        attend_gain,
        query_weight,
        cache_keys,
        cache_values,
        head_lambda,
        head_gain,
        output_weight,
        mixer_gain,
        gate_weight,
        up_weight,
        down_weight,
    ) = arrays
    rows, local = tokens.shape
    positions, kv_local = cache_keys.shape[1:3]
    heads = head_lambda.shape[0]
    assert kv_local == 1
    hidden = gate_weight.shape[1]
    n_pieces = min(2, n_kv)
    tiles = hidden // n_pieces // LANES
    assert tiles * n_pieces * LANES == hidden
    widths = [(tiles + 1) // 2 * LANES, tiles // 2 * LANES]
    count = rows * 2 * heads
    query_width = query_weight.shape[1]
    partners = max(n_tp - 1, 1)
    buffers = [2 * widths[0] + LANES, 2 * widths[1]]
    phases = 6 + 2 * len(widths)
    operands = (
        tokens,
        attend_gain.reshape(1, -1),
        query_weight,
        cache_keys.reshape(rows, positions, -1),
        cache_values.reshape(rows, positions, -1),
        head_lambda.reshape(1, -1),
        head_gain.reshape(1, -1),
        output_weight,
        mixer_gain.reshape(1, -1),
        gate_weight,
        up_weight,
        down_weight,
        jnp.asarray(rope_table(positions * n_kv)),
    )
    loaded = [pltpu.VMEM(a.shape, a.dtype) for a in operands]
    return pl.pallas_call(
        functools.partial(kernel, n_kv, n_tp, n_pieces, widths, local * n_kv),
        out_shape=jax.ShapeDtypeStruct(tokens.shape, tokens.dtype),
        in_specs=[pl.BlockSpec(memory_space=pl.ANY)] * len(operands),
        out_specs=pl.BlockSpec(memory_space=pltpu.VMEM),
        scratch_shapes=loaded
        + [
            pltpu.VMEM((rows, query_width + LANES), BF16),
            pltpu.VMEM((n_kv, rows, query_width + LANES), BF16),
            pltpu.VMEM((count, LANES), BF16),
            pltpu.VMEM((n_kv, count, LANES), BF16),
            pltpu.VMEM((2, count), F32),
            pltpu.VMEM((n_kv, 2, count), F32),
            pltpu.VMEM((rows, local), BF16),
            pltpu.VMEM((partners, rows, local), BF16),
            [pltpu.VMEM((n_pieces, rows, size), BF16) for size in buffers],
            [pltpu.VMEM((n_kv, rows, size), BF16) for size in buffers],
            [pltpu.VMEM((n_pieces, rows, size), BF16) for size in widths],
            pltpu.VMEM((rows, local), BF16),
            pltpu.VMEM((partners, rows, local), BF16),
            pltpu.VMEM((heads * rows, LANES), F32),
            pltpu.VMEM((heads * rows, LANES), F32),
            pltpu.SemaphoreType.DMA((len(operands),)),
            pltpu.SemaphoreType.DMA((phases, n_kv)),
            pltpu.SemaphoreType.DMA((phases, n_kv)),
            pltpu.SemaphoreType.DMA((n_pieces, len(widths))),
            pltpu.SemaphoreType.DMA((2, partners)),
            pltpu.SemaphoreType.DMA((2, partners)),
        ],
        compiler_params=pltpu.CompilerParams(
            collective_id=0, has_side_effects=True
        ),
    )(*operands)


def solution(mesh):
    return jax.shard_map(
        functools.partial(on_device, mesh.shape["kv"], mesh.shape["tp"]),
        mesh=mesh,
        in_specs=(
            P(("grp", "dp"), "kv"),
            P("kv"),
            P("kv", "tp"),
            P(("grp", "dp"), "kv", "tp", None),
            P(("grp", "dp"), "kv", "tp", None),
            P("tp"),
            P(),
            P("tp", "kv"),
            P("kv"),
            P("kv", "tp"),
            P("kv", "tp"),
            P("tp", "kv"),
        ),
        out_specs=P(("grp", "dp"), "kv"),
        check_vma=False,
    )
```

```python
import functools

import jax
import jax.numpy as jnp
import numpy as np
from jax import lax
from jax.experimental import pallas as pl
from jax.experimental.pallas import tpu as pltpu
from jax.sharding import PartitionSpec as P

HD = 64
ROPE_BASE = 500000.0
EPSILON = 1e-06
KEEP_SCALE = 0.8
LANES = 128
B_PARTS = 4
F32 = jnp.float32
BF16 = jnp.bfloat16


def high_low(column):
    high = column.astype(BF16).astype(F32)
    low = column - high
    lane = lax.broadcasted_iota(jnp.int32, (column.shape[0], LANES), 1)
    return jnp.where(lane < LANES // 2, high, low).astype(BF16)


def from_high_low(tile):
    tile = tile.astype(F32)
    return tile[:, 0:1] + tile[:, LANES // 2 : LANES // 2 + 1]


def kernel(
    n_kv,
    n_tp,
    n_pieces,
    widths,
    features,
    tok_hbm,
    again_hbm,
    wq_hbm,
    key_hbm,
    val_hbm,
    lam_hbm,
    hgain_hbm,
    wo_hbm,
    mgain_hbm,
    wg_hbm,
    wu_hbm,
    wd_hbm,
    rope_hbm,
    out_ref,
    tok,
    again,
    wq,
    keys,
    vals,
    lam,
    hgain,
    wo,
    mgain,
    wg,
    wu,
    wd,
    rope,
    a_send,
    a_recv,
    b_send,
    b_recv,
    s_send,
    s_recv,
    c_send,
    c_recv,
    d_sends,
    d_recvs,
    e_alls,
    f_send,
    f_recv,
    query_rows,
    head_rows,
    load_sem,
    kv_send,
    kv_recv,
    piece_send,
    tp_send,
    tp_recv,
):
    me = lax.axis_index("kv")
    core = lax.axis_index("tp")
    rows = tok.shape[0]
    heads = lam.shape[1]
    hidden_here = wg_hbm.shape[1]

    loads = []
    for index, (source, target) in enumerate(
        [
            (tok_hbm, tok),
            (again_hbm, again),
            (wq_hbm, wq),
            (rope_hbm, rope),
            (lam_hbm, lam),
            (hgain_hbm, hgain),
            (mgain_hbm, mgain),
            (key_hbm, keys),
            (val_hbm, vals),
            (wo_hbm, wo),
            (wg_hbm, wg),
            (wu_hbm, wu),
            (wd_hbm, wd),
        ]
    ):
        copy = pltpu.make_async_copy(source, target, load_sem.at[index])
        copy.start()
        loads.append(copy)

    barrier = pltpu.get_barrier_semaphore()
    for k in range(1, n_kv):
        pl.semaphore_signal(
            barrier,
            inc=1,
            device_id={"kv": lax.rem(me + k, n_kv)},
            device_id_type=pl.DeviceIdType.MESH,
        )
    for k in range(1, n_tp):
        pl.semaphore_signal(
            barrier,
            inc=1,
            device_id={"tp": lax.rem(core + k, n_tp)},
            device_id_type=pl.DeviceIdType.MESH,
        )

    pending = []
    half = max(n_kv // 2, 1)
    on_left = me < half

    def far_first(j):
        below, above = n_kv - 1 - j, j
        below = jnp.where(below > me, below, below - 1)
        above = jnp.where(above < me, above, above + 1)
        return jnp.where(on_left, below, above)

    peers = [far_first(j) for j in range(n_kv - 1)]

    def kv_copy(phase, source, target, slot_sent, slot_received, peer):
        return pltpu.make_async_remote_copy(
            src_ref=source,
            dst_ref=target,
            send_sem=kv_send.at[phase, slot_sent],
            recv_sem=kv_recv.at[phase, slot_received],
            device_id={"kv": peer},
            device_id_type=pl.DeviceIdType.MESH,
        )

    def to_all(phase, source, landing):
        for j, peer in enumerate(peers):
            copy = kv_copy(phase, source, landing(me), j, me, peer)
            copy.start()
            pending.append(copy)

    def from_kv(phase, landing, origin):
        kv_copy(phase, landing, landing, 0, origin, origin).wait_recv()

    def to_tp(phase, k, source, target):
        copy = pltpu.make_async_remote_copy(
            src_ref=source,
            dst_ref=target,
            send_sem=tp_send.at[phase, k - 1],
            recv_sem=tp_recv.at[phase, k - 1],
            device_id={"tp": lax.rem(core + k, n_tp)},
            device_id_type=pl.DeviceIdType.MESH,
        )
        copy.start()
        pending.append(copy)
        return copy

    for index in (0, 1, 2):
        loads[index].wait()
    tok_float = tok[...].astype(F32)
    scaled = (tok_float * again[...]).astype(BF16)
    query_part = jnp.dot(scaled, wq[...], preferred_element_type=F32)
    squares = jnp.sum(tok_float * tok_float, axis=1, keepdims=True)
    query_width = wq.shape[1]
    a_send[:, :query_width] = query_part.astype(BF16)
    a_send[:, query_width:] = high_low(squares)
    pl.semaphore_wait(barrier, n_kv - 1 + n_tp - 1)
    to_all(0, a_send, lambda slot: a_recv.at[slot])
    for index in (3, 4, 5, 6, 7):
        loads[index].wait()
    for peer in reversed(peers):
        from_kv(0, a_recv.at[peer], peer)
        query_part = query_part + a_recv[peer, :, :query_width].astype(F32)
        squares = squares + from_high_low(a_recv[peer, :, query_width:])
    query = query_part * lax.rsqrt(squares / features + EPSILON)

    lane = lax.broadcasted_iota(jnp.int32, (rows, LANES), 1)
    lower = lax.rem(lane, HD) < HD // 2
    cosine = rope[0:1, :]
    sine = rope[1:2, :]
    for h in range(heads):
        block = query[:, h * LANES : (h + 1) * LANES]
        partner = jnp.where(
            lower,
            pltpu.roll(block, LANES - HD // 2, 1),
            pltpu.roll(block, HD // 2, 1),
        )
        query_rows[h * rows : (h + 1) * rows, :] = block * cosine + partner * sine

    head_lane = lax.broadcasted_iota(jnp.int32, (heads, LANES), 1)
    scores = []
    for b in range(rows):
        turned = query_rows[pl.ds(b, heads, stride=rows), :]
        rounded = turned.astype(BF16).astype(F32) * HD ** (-0.5)
        both = jnp.concatenate(
            [
                jnp.where(head_lane < HD, rounded, 0.0),
                jnp.where(head_lane < HD, 0.0, rounded),
            ],
            axis=0,
        ).astype(BF16)
        scores.append(
            lax.dot_general(
                both, keys[b], (((1,), (1,)), ((), ())), preferred_element_type=F32
            )
        )
    loads[8].wait()
    count = 2 * heads
    all_rows = rows * count
    weighted, row_max, row_total = [], [], []
    for b in range(rows):
        top = jnp.max(scores[b], axis=1, keepdims=True)
        exponent = jnp.exp(scores[b] - top)
        row_max.append(top)
        row_total.append(jnp.sum(exponent, axis=1, keepdims=True))
        own = jnp.dot(exponent.astype(BF16), vals[b], preferred_element_type=F32)
        b_send[b * count : (b + 1) * count, :] = own.astype(BF16)
        weighted.append(own)
        if (b + 1) % (rows // B_PARTS) == 0:
            part = b // (rows // B_PARTS)
            span = pl.ds(part * (all_rows // B_PARTS), all_rows // B_PARTS)
            to_all(1 + part, b_send.at[span], lambda slot: b_recv.at[slot, span])
    diagonal = lax.broadcasted_iota(jnp.int32, (all_rows, all_rows), 0) == (
        lax.broadcasted_iota(jnp.int32, (all_rows, all_rows), 1)
    )

    def to_lanes(column):
        return jnp.sum(jnp.where(diagonal, column, 0.0), axis=0, keepdims=True)

    def to_rows(line):
        return jnp.sum(jnp.where(diagonal, line, 0.0), axis=1, keepdims=True)

    own_max = to_lanes(jnp.concatenate(row_max, axis=0))
    own_total = to_lanes(jnp.concatenate(row_total, axis=0))
    s_send[0:1, :] = own_max
    s_send[1:2, :] = own_total
    to_all(5, s_send, lambda slot: s_recv.at[slot])
    weighted = jnp.concatenate(weighted, axis=0)
    eye = lax.broadcasted_iota(jnp.int32, (heads, heads), 0) == (
        lax.broadcasted_iota(jnp.int32, (heads, heads), 1)
    )
    lam_column = jnp.sum(jnp.where(eye, lam[...], 0.0), axis=1, keepdims=True)
    for peer in reversed(peers):
        from_kv(5, s_recv.at[peer], peer)
    maxima = [own_max] + [s_recv[peer, 0:1, :] for peer in reversed(peers)]
    totals = [own_total] + [s_recv[peer, 1:2, :] for peer in reversed(peers)]
    joint = functools.reduce(jnp.maximum, maxima)
    factors = [jnp.exp(m - joint) for m in maxima]
    total = functools.reduce(jnp.add, [f * t for f, t in zip(factors, totals)])
    averaged = weighted * to_rows(factors[0] / total)
    shares = [to_rows(f / total) for f in factors[1:]]
    for share, peer in zip(shares, reversed(peers)):
        for part in range(B_PARTS):
            span = pl.ds(part * (all_rows // B_PARTS), all_rows // B_PARTS)
            from_kv(1 + part, b_recv.at[peer, span], peer)
        averaged = averaged + b_recv[peer].astype(F32) * share
    averaged = averaged.reshape(rows, 2, heads, LANES)
    difference = averaged[:, 0] - lam_column[None] * averaged[:, 1]
    normed = difference * lax.rsqrt(
        jnp.mean(difference * difference, axis=-1, keepdims=True) + EPSILON
    )
    normed = normed * (hgain[...] * KEEP_SCALE)[None]
    head_rows[...] = normed.reshape(rows * heads, LANES)
    heads_out = jnp.concatenate(
        [head_rows[pl.ds(h, rows, stride=heads), :] for h in range(heads)], axis=1
    ).astype(BF16)

    loads[9].wait()
    attended = jnp.dot(heads_out, wo[...], preferred_element_type=F32).astype(BF16)
    c_send[...] = attended
    copies = [to_tp(0, k, c_send, c_recv.at[k - 1]) for k in range(1, n_tp)]
    attended = attended.astype(F32)
    for index in (10, 11):
        loads[index].wait()
    for k, copy in enumerate(copies):
        copy.wait_recv()
        attended = attended + c_recv[k].astype(F32)
    mid_float = (tok_float + attended).astype(BF16).astype(F32)
    mixer_in = (mid_float * mgain[...]).astype(BF16)
    squares = jnp.sum(mid_float * mid_float, axis=1, keepdims=True)

    square_tile = high_low(squares)
    near = jnp.where(on_left, 0, n_pieces - 1)
    far = n_pieces - 1 - near
    first = (n_kv - n_pieces) // 2
    reduces = jnp.logical_and(me >= first, me < first + n_pieces)
    span = hidden_here // n_pieces
    starts = [sum(widths[:j]) for j in range(len(widths))]
    grids = list(zip(d_sends, d_recvs, e_alls, widths, starts))
    d_copies = []
    for piece in ([far] if n_pieces > 1 else []) + [near]:
        target = first + piece
        for j, (d_send, d_recv, _, width, start) in enumerate(grids):
            columns = pl.ds(pl.multiple_of(piece * span + start, LANES), width)
            gate = jnp.dot(mixer_in, wg[:, columns], preferred_element_type=F32)
            d_send[piece, :, :width] = gate.astype(BF16)
            up = jnp.dot(mixer_in, wu[:, columns], preferred_element_type=F32)
            d_send[piece, :, width : 2 * width] = up.astype(BF16)
            if j == 0:
                d_send[piece, :, 2 * width :] = square_tile
            copy = pltpu.make_async_remote_copy(
                src_ref=d_send.at[piece],
                dst_ref=d_recv.at[me],
                send_sem=piece_send.at[piece, j],
                recv_sem=kv_recv.at[6 + j, me],
                device_id={"kv": target},
                device_id_type=pl.DeviceIdType.MESH,
            )
            d_copies.append((target, copy))
            pl.when(me != target)(copy.start)

    e_phase = 6 + len(widths)

    @pl.when(reduces)
    def _():
        own = me - first
        row_squares = squares
        for j, (d_send, d_recv, e_all, width, _) in enumerate(grids):
            gate = d_send[own, :, :width].astype(F32)
            up = d_send[own, :, width : 2 * width].astype(F32)
            for peer in reversed(peers):
                from_kv(6 + j, d_recv.at[peer], peer)
                gate = gate + d_recv[peer, :, :width].astype(F32)
                up = up + d_recv[peer, :, width : 2 * width].astype(F32)
                if j == 0:
                    row_squares = row_squares + from_high_low(
                        d_recv[peer, :, 2 * width :]
                    )
            mixer_scale = lax.rsqrt(row_squares / features + EPSILON)
            gate = gate * mixer_scale
            up = up * mixer_scale
            e_all[own] = (gate / (1.0 + jnp.exp(-gate)) * up).astype(BF16)
            for i, peer in enumerate(peers):
                kv_copy(e_phase + j, e_all.at[own], e_all.at[own], i, own, peer).start()

    loads[12].wait()
    projected = jnp.zeros((rows, wd.shape[1]), F32)
    for j, (_, _, e_all, width, start) in enumerate(grids):
        for piece in [near] + ([far] if n_pieces > 1 else []):
            arrival = kv_copy(e_phase + j, e_all.at[piece], e_all.at[piece], 0, piece, me)
            pl.when(me != first + piece)(arrival.wait_recv)
            part = wd[pl.ds(pl.multiple_of(piece * span + start, LANES), width), :]
            projected = projected + jnp.dot(
                e_all[piece], part, preferred_element_type=F32
            )
    projected = projected.astype(BF16)
    f_send[...] = projected
    copies = [to_tp(1, k, f_send, f_recv.at[k - 1]) for k in range(1, n_tp)]
    mixed = projected.astype(F32)
    for k, copy in enumerate(copies):
        copy.wait_recv()
        mixed = mixed + f_recv[k].astype(F32)
    out_ref[...] = (mid_float + mixed).astype(BF16)
    for copy in pending:
        copy.wait_send()
    for target, copy in d_copies:
        pl.when(me != target)(copy.wait_send)

    @pl.when(reduces)
    def _():
        own = me - first
        for j, (_, _, e_all, _, _) in enumerate(grids):
            for i, peer in enumerate(peers):
                kv_copy(e_phase + j, e_all.at[own], e_all.at[own], i, own, peer).wait_send()


def rope_table(context):
    half = HD // 2
    frequency = (ROPE_BASE ** (-np.arange(half) * 2.0 / HD)).astype(np.float32)
    angles = (np.float32(context) * frequency).astype(np.float64)
    cosine = np.tile(np.cos(angles), LANES // half)
    sine = np.tile(np.concatenate([-np.sin(angles), np.sin(angles)]), LANES // HD)
    return np.stack([cosine, sine]).astype(np.float32)


def on_device(n_kv, n_tp, *arrays):
    (
        tokens,
        attend_gain,
        query_weight,
        cache_keys,
        cache_values,
        head_lambda,
        head_gain,
        output_weight,
        mixer_gain,
        gate_weight,
        up_weight,
        down_weight,
    ) = arrays
    rows, local = tokens.shape
    positions, kv_local = cache_keys.shape[1:3]
    heads = head_lambda.shape[0]
    assert kv_local == 1
    hidden = gate_weight.shape[1]
    n_pieces = min(2, n_kv)
    tiles = hidden // n_pieces // LANES
    assert tiles * n_pieces * LANES == hidden
    widths = [(tiles + 1) // 2 * LANES, tiles // 2 * LANES]
    count = rows * 2 * heads
    query_width = query_weight.shape[1]
    partners = max(n_tp - 1, 1)
    buffers = [2 * widths[0] + LANES, 2 * widths[1]]
    phases = 6 + 2 * len(widths)
    operands = (
        tokens,
        attend_gain.reshape(1, -1),
        query_weight,
        cache_keys.reshape(rows, positions, -1),
        cache_values.reshape(rows, positions, -1),
        head_lambda.reshape(1, -1),
        head_gain.reshape(1, -1),
        output_weight,
        mixer_gain.reshape(1, -1),
        gate_weight,
        up_weight,
        down_weight,
        jnp.asarray(rope_table(positions * n_kv)),
    )
    loaded = [pltpu.VMEM(a.shape, a.dtype) for a in operands]
    return pl.pallas_call(
        functools.partial(kernel, n_kv, n_tp, n_pieces, widths, local * n_kv),
        out_shape=pltpu.VMEM(tokens.shape, tokens.dtype),
        in_specs=[pl.BlockSpec(memory_space=pl.ANY)] * len(operands),
        out_specs=pl.BlockSpec(memory_space=pltpu.VMEM),
        scratch_shapes=loaded
        + [
            pltpu.VMEM((rows, query_width + LANES), BF16),
            pltpu.VMEM((n_kv, rows, query_width + LANES), BF16),
            pltpu.VMEM((count, LANES), BF16),
            pltpu.VMEM((n_kv, count, LANES), BF16),
            pltpu.VMEM((2, count), F32),
            pltpu.VMEM((n_kv, 2, count), F32),
            pltpu.VMEM((rows, local), BF16),
            pltpu.VMEM((partners, rows, local), BF16),
            [pltpu.VMEM((n_pieces, rows, size), BF16) for size in buffers],
            [pltpu.VMEM((n_kv, rows, size), BF16) for size in buffers],
            [pltpu.VMEM((n_pieces, rows, size), BF16) for size in widths],
            pltpu.VMEM((rows, local), BF16),
            pltpu.VMEM((partners, rows, local), BF16),
            pltpu.VMEM((heads * rows, LANES), F32),
            pltpu.VMEM((heads * rows, LANES), F32),
            pltpu.SemaphoreType.DMA((len(operands),)),
            pltpu.SemaphoreType.DMA((phases, n_kv)),
            pltpu.SemaphoreType.DMA((phases, n_kv)),
            pltpu.SemaphoreType.DMA((n_pieces, len(widths))),
            pltpu.SemaphoreType.DMA((2, partners)),
            pltpu.SemaphoreType.DMA((2, partners)),
        ],
        compiler_params=pltpu.CompilerParams(
            collective_id=0, has_side_effects=True
        ),
    )(*operands)


def solution(mesh):
    return jax.shard_map(
        functools.partial(on_device, mesh.shape["kv"], mesh.shape["tp"]),
        mesh=mesh,
        in_specs=(
            P(("grp", "dp"), "kv"),
            P("kv"),
            P("kv", "tp"),
            P(("grp", "dp"), "kv", "tp", None),
            P(("grp", "dp"), "kv", "tp", None),
            P("tp"),
            P(),
            P("tp", "kv"),
            P("kv"),
            P("kv", "tp"),
            P("kv", "tp"),
            P("tp", "kv"),
        ),
        out_specs=P(("grp", "dp"), "kv"),
        check_vma=False,
    )
```
